128 devices in a mesh: fs: 32 (over z, y, core), tp: 4 (over x).
Axes of the slice: x: 4, y: 4, z: 4, core: 2. Of those that a mesh axis runs over, the one named last changes fastest.
Arguments:
- model_input: bfloat16 [65536, 2048], P('fs'), may hold values from -6 to 6
- value_cotan: bfloat16 [65536, 2048], P('fs', 'tp'), may hold values from -0.0234375 to 0.0234375
- mixer_cotan: bfloat16 [65536, 2048], P('fs'), may hold values from -0.0234375 to 0.0234375
- head_output: bfloat16 [65536, 2048], P('fs', 'tp'), may hold values from -6 to 6
- value_weight: float32 [2048, 2048], P('fs', 'tp'), may hold values from -0.125 to 0.125
- value_factor: bfloat16 [2048, 512], P('fs'), may hold values from -0.125 to 0.125
- value_first: float32 [512, 2048], P('fs', 'tp'), may hold values from -3 to 3
- value_second: float32 [512, 2048], P('fs', 'tp'), may hold values from 0.02 to 0.5
- output_weight: float32 [2048, 2048], P('fs', 'tp'), may hold values from -0.125 to 0.125
- output_factor: bfloat16 [2048, 512], P('fs'), may hold values from -0.125 to 0.125
- output_first: float32 [512, 2048], P('fs', 'tp'), may hold values from -3 to 3
- output_second: float32 [512, 2048], P('fs', 'tp'), may hold values from 0.02 to 0.5
Outputs:
- value_step: float32 [2048, 2048], P('fs', 'tp')
- value_updated: float32 [2048, 2048], P('fs', 'tp')
- value_first_new: float32 [512, 2048], P('fs', 'tp')
- value_second_new: float32 [512, 2048], P('fs', 'tp')
- value_copy: bfloat16 [2048, 2048], P(None, 'tp')
- output_step: float32 [2048, 2048], P('fs', 'tp')
- output_updated: float32 [2048, 2048], P('fs', 'tp')
- output_first_new: float32 [512, 2048], P('fs', 'tp')
- output_second_new: float32 [512, 2048], P('fs', 'tp')
- output_copy: bfloat16 [2048, 2048], P(None, 'tp')
The draws below stay inside these ranges and needn't reach their ends.
All inputs are finite; a program needn't handle non-finite values.
Results may differ from the reference program's by a relative error of at most 0.0059.
Values may be sent and summed in bfloat16 or wider, within the bound.
A program may use at most 128 MiB of HBM per device.

```python
import math
import jax
import jax.numpy as jnp
from jax import lax

D = 2048
RANK = 512
TOK_DEV = 2048
HV = 2048
TOKENS = 65536
N_FS = 32


def with_spikes(array, stream_key, source, target, blocks, factor):
    def block_of(dim):
        return (jnp.arange(array.shape[dim]) // (array.shape[dim] // blocks)).reshape((-1,) + (1,) * (array.ndim - 1 - dim))

    near = jax.random.permutation(stream_key, blocks)[block_of(target)]
    second = (block_of(target) + blocks // 2) % blocks
    return jnp.where((block_of(source) == near) | (block_of(source) == second), factor * array, array)


def steps_of(stream_key, extent, shards, low, high):
    level, own = 1.0, jax.random.fold_in(stream_key, 6)
    for position, shards_of in shards:
        steps = jnp.exp(jax.random.uniform(jax.random.fold_in(own, position), (shards_of,), jnp.float32, low / len(shards), high / len(shards)))
        level = level * jnp.repeat(steps, extent[position] // shards_of).reshape([-1 if axis == position else 1 for axis in range(len(extent))])
    return level


def bell_draw(own_key, extent, spread, limit, shards=(), dtype=jnp.bfloat16):
    array = jax.random.normal(own_key, extent, jnp.float32) * spread
    if len(shards) > 0:
        array = steps_of(own_key, extent, shards, -0.22, 0.18) * array
    return jnp.clip(array, min=-limit, max=limit).astype(dtype)


def noise_with(own_key, extent, spread, bound, cuts, heavy, kind=jnp.bfloat16):
    result = spread * jax.random.normal(own_key, extent, jnp.float32)
    if cuts:
        result = result * steps_of(own_key, extent, cuts, -0.22, 0.18)
    return jnp.clip(with_spikes(result, jax.random.fold_in(own_key, 3), *heavy), -bound, bound).astype(kind)


def setup_inputs(seed: int = 0) -> dict:
    arg_keys = jax.random.split(jax.random.key(seed), 13)
    model_input = noise_with(arg_keys[0], (TOKENS, D), 1.0, 6.0, ((0, 32),), (0, 1, 32, 2.75))
    value_cotan = bell_draw(arg_keys[1], (TOKENS, HV), ((TOK_DEV * N_FS) ** -0.5), 0.0234375, ((0, 32), (1, 4)))
    mixer_cotan = noise_with(arg_keys[2], (TOKENS, D), ((TOK_DEV * N_FS) ** -0.5), 0.0234375, ((0, 32),), (0, 1, 32, 2.75))
    head_output = bell_draw(arg_keys[3], (TOKENS, HV), 1.0, 6.0, ((0, 32), (1, 4)))
    value_weight = bell_draw(arg_keys[4], (D, HV), D ** -0.5, 0.125, ((0, 32), (1, 4)), jnp.float32)
    value_factor = bell_draw(arg_keys[5], (D, RANK), D ** -0.5, 0.125, ((0, 32),))
    value_first = bell_draw(arg_keys[6], (RANK, HV), 0.5, 3.0, ((0, 32), (1, 4)), jnp.float32)
    value_second = jnp.clip(jnp.exp(math.log(0.5) - 3.218876 * jax.random.uniform(arg_keys[7], (RANK, HV), jnp.float32) ** steps_of(arg_keys[7], (RANK, HV), ((0, 32), (1, 4)), -0.2, 0.2)), 0.02, 0.5)
    output_weight = bell_draw(arg_keys[8], (D, HV), HV ** -0.5, 0.125, ((0, 32), (1, 4)), jnp.float32)
    output_factor = bell_draw(arg_keys[9], (D, RANK), D ** -0.5, 0.125, ((0, 32),))
    output_first = bell_draw(arg_keys[10], (RANK, HV), 0.5, 3.0, ((0, 32), (1, 4)), jnp.float32)
    output_second = jnp.clip(jnp.exp(math.log(0.5) - 3.218876 * jax.random.uniform(arg_keys[11], (RANK, HV), jnp.float32) ** steps_of(arg_keys[11], (RANK, HV), ((0, 32), (1, 4)), -0.2, 0.2)), 0.02, 0.5)
    return dict(model_input=model_input, value_cotan=value_cotan, mixer_cotan=mixer_cotan, head_output=head_output, value_weight=value_weight, value_factor=value_factor, value_first=value_first, value_second=value_second, output_weight=output_weight, output_factor=output_factor, output_first=output_first, output_second=output_second)


beta_first = 0.8
beta_second = 0.9
step_rate = 0.02
scale_floor = 0.25
tiny_eps = 1e-08

def low_rank(rows_in, cols_in, factor, first_moment, second_moment):
    gradient = jnp.dot(rows_in.T, cols_in, preferred_element_type=jnp.float32)
    projected = jnp.dot(factor.astype(jnp.float32).T, gradient, precision=lax.Precision.HIGHEST)
    first_new = beta_first * first_moment + (1.0 - beta_first) * projected
    second_new = beta_second * second_moment + (1.0 - beta_second) * projected * projected
    direction = (first_new / (jnp.sqrt(second_new) + tiny_eps)).astype(jnp.bfloat16)
    expanded = jnp.dot(factor, direction, preferred_element_type=jnp.float32)
    return (expanded, first_new, second_new)

def finish(expanded, weight):
    mean_square = jnp.sum(expanded * expanded) / (D * HV)
    update_step = step_rate / jnp.sqrt(mean_square + scale_floor) * expanded
    updated = weight - update_step
    return (update_step, updated, updated.astype(jnp.bfloat16))

def reference(model_input, value_cotan, mixer_cotan, head_output, value_weight, value_factor, value_first, value_second, output_weight, output_factor, output_first, output_second):
    value_exp, value_fnew, value_snew = low_rank(model_input, value_cotan, value_factor, value_first, value_second)
    output_exp, output_fnew, output_snew = low_rank(mixer_cotan, head_output, output_factor, output_first, output_second)
    value_step, value_updated, value_copy = finish(value_exp, value_weight)
    output_step, output_updated, output_copy = finish(output_exp, output_weight)
    return (value_step, value_updated, value_fnew, value_snew, value_copy, output_step, output_updated, output_fnew, output_snew, output_copy)
```

```python
import functools

import jax
import jax.numpy as jnp
from jax import lax
from jax.experimental import pallas as pl
from jax.experimental.pallas import tpu as pltpu
from jax.sharding import Mesh
from jax.sharding import PartitionSpec as P

D = 2048
HV = 2048
FS = ("z", "y", "c")
MESH = pl.DeviceIdType.MESH

beta_first = 0.8
beta_second = 0.9
step_rate = 0.02
scale_floor = 0.25
tiny_eps = 1e-08

BF = jnp.bfloat16
F32 = jnp.float32


def exchange_kernel(
    rows0, cols0, rows1, cols1, w0, w1, f0, f1, a0, b0, a1, b1,
    E, W, mom, ss,
    rows, cols, colsT, gT, F, wf, mo, Pj, X, S, R, Dr, XR,
    in_sem, g_send, g_recv, d_send, d_recv, s_send, s_recv, x_send, x_recv,
):
    z, y, c, x = (lax.axis_index(n) for n in ("z", "y", "c", "x"))
    chip = z * 4 + y
    other = 1 - c
    ra = y + c * (z - y)
    rb = z + c * (y - z)

    def place(a, b):
        zz = b + c * (a - b)
        yy = a + c * (b - a)
        return zz, yy

    def shard(a, b):
        zz, yy = place(a, b)
        return (zz * 4 + yy) * 2 + c

    def at(a, b):
        zz, yy = place(a, b)
        return {"z": zz, "y": yy}

    def plus(v, k):
        return lax.rem(v + k, 4)

    def remote(src, dst, ssem, rsem, dev):
        return pltpu.make_async_remote_copy(
            src_ref=src, dst_ref=dst, send_sem=ssem, recv_sem=rsem,
            device_id=dev, device_id_type=MESH,
        )

    partner = {"c": other}

    bar = pltpu.get_barrier_semaphore()
    peers = [{"z": plus(z, k // 4), "y": plus(y, k % 4)} for k in range(1, 16)]
    xpeers = [{"x": plus(x, k)} for k in range(1, 4)]
    for p in peers + [partner] + xpeers:
        pl.semaphore_signal(bar, inc=1, device_id=p, device_id_type=MESH)

    me = chip * 2 + c
    fin = [pltpu.make_async_copy(f, F.at[m, me], in_sem.at[m]) for m, f in enumerate((f0, f1))]
    win = [pltpu.make_async_copy(w, wf.at[m], in_sem.at[2 + m]) for m, w in enumerate((w0, w1))]
    cin = [pltpu.make_async_copy(v, cols.at[m], in_sem.at[4 + m]) for m, v in enumerate((cols0, cols1))]
    rin = [
        [
            pltpu.make_async_copy(
                v.at[:, pl.ds(512 * j, 512)], rows.at[m, j], in_sem.at[6 + 4 * m + j]
            )
            for j in range(4)
        ]
        for m, v in enumerate((rows0, rows1))
    ]
    min_ = [
        pltpu.make_async_copy(v, mo.at[i], in_sem.at[14 + i]) for i, v in enumerate((a0, b0, a1, b1))
    ]
    for cp in fin + [cin[0]] + rin[0] + win + [cin[1]] + rin[1] + min_:
        cp.start()

    def G(p):
        return (F if p < 2 else W).at[p % 2]

    am, ap, af = plus(ra, 3), plus(ra, 1), plus(ra, 2)
    bm, bp, bf = plus(rb, 3), plus(rb, 1), plus(rb, 2)
    LO, HI = pl.ds(0, 32), pl.ds(32, 32)

    def send(p, s, dev, k, half=None):
        ref = G(p).at[s] if half is None else G(p).at[s, half]
        remote(ref, ref, g_send.at[p], g_recv.at[p, k], dev).start()

    def arrived(p, k, n):
        ref = G(p).at[pl.ds(0, n)]
        remote(ref, ref, g_send.at[p], g_recv.at[p, k], partner).wait_recv()

    def across(p, s):
        send(p, s, partner, 10)

    def gather_step(p, step):
        if step == 0:
            s = shard(ra, rb)
            send(p, s, at(ap, rb), 0)
            send(p, s, at(am, rb), 1)
            send(p, s, at(ra, bp), 3)
            send(p, s, at(ra, bm), 4)
            across(p, s)
        if step == 1:
            arrived(p, 0, 1)
            send(p, shard(am, rb), at(ap, rb), 2, LO)
            arrived(p, 1, 1)
            send(p, shard(ap, rb), at(am, rb), 2, HI)
            for a in (am, ap):
                send(p, shard(a, rb), at(ra, bp), 5)
                send(p, shard(a, rb), at(ra, bm), 6)
            arrived(p, 3, 1)
            send(p, shard(ra, bm), at(ra, bp), 9, LO)
            arrived(p, 4, 1)
            send(p, shard(ra, bp), at(ra, bm), 9, HI)
            for s in (shard(am, rb), shard(ap, rb), shard(ra, bm), shard(ra, bp)):
                across(p, s)
        if step == 2:
            arrived(p, 2, 1)
            send(p, shard(af, rb), at(ra, bp), 7)
            send(p, shard(af, rb), at(ra, bm), 8)
            arrived(p, 5, 2)
            for a in (am, ap):
                send(p, shard(a, bm), at(ra, bp), 9, LO)
            arrived(p, 6, 2)
            for a in (am, ap):
                send(p, shard(a, bp), at(ra, bm), 9, HI)
            across(p, shard(af, rb))
            for a in (am, ap):
                across(p, shard(a, bm))
                across(p, shard(a, bp))
        if step == 3:
            arrived(p, 7, 1)
            send(p, shard(af, bm), at(ra, bp), 9, LO)
            arrived(p, 8, 1)
            send(p, shard(af, bp), at(ra, bm), 9, HI)
            across(p, shard(af, bm))
            across(p, shard(af, bp))
        if step == 4:
            arrived(p, 9, 4)
            for a in (ra, am, ap, af):
                across(p, shard(a, bf))
        if step == 5:
            arrived(p, 10, 16)

    def gather_sent(p):
        ref = G(p).at[pl.ds(0, 31)]
        remote(ref, ref, g_send.at[p], g_recv.at[p, 0], partner).wait_send()

    def transpose_cols(m):
        cin[m].wait()
        for t in range(4):
            colsT[m, :, 512 * t : 512 * t + 512] = cols[m, 512 * t : 512 * t + 512, :].T

    def grad_chunk(m, j):
        rin[m][j].wait()
        out = jnp.dot(colsT[m], rows[m, j], preferred_element_type=F32)
        gT[m, :, 512 * j : 512 * j + 512] = out.astype(BF)

    def project(m):
        for n in range(2):
            f = F[m, :, :, 256 * n : 256 * n + 256].reshape(D, 256)
            out = jnp.dot(gT[m], f, preferred_element_type=F32)
            Pj[m, 8 * n : 8 * n + 8] = out.T.astype(BF).reshape(8, 2, 16, 512)
        remote(Pj.at[m, :, other], X.at[m], d_send.at[m], d_recv.at[m], partner).start()

    def scatter(m):
        remote(Pj.at[m, :, other], X.at[m], d_send.at[m], d_recv.at[m], partner).wait_recv()
        S[m] = (Pj[m, :, c].astype(F32) + X[m].astype(F32)).astype(BF)
        for k in (10, 9, 11, 6, 14, 2, 8, 5, 7, 13, 15, 1, 3, 4, 12):
            zz, yy = plus(z, k // 4), plus(y, k % 4)
            remote(
                S.at[m, zz * 4 + yy], R.at[m, k - 1], s_send.at[m], s_recv.at[m],
                {"z": zz, "y": yy},
            ).start()

    def moments(m):
        remote(R.at[m], R.at[m], s_send.at[m], s_recv.at[m], partner).wait_recv()
        proj = S[m, chip].astype(F32) + jnp.sum(R[m].astype(F32), axis=0)
        fnew = beta_first * mo[2 * m] + (1.0 - beta_first) * proj
        snew = beta_second * mo[2 * m + 1] + (1.0 - beta_second) * proj * proj
        mom[m, 0] = fnew
        mom[m, 1] = snew
        Dr[m, chip, c] = (fnew / (jnp.sqrt(snew) + tiny_eps)).astype(BF)
        ref = Dr.at[m, chip, c]
        for k in (10, 9, 11, 6, 14, 2, 8, 5, 7, 13, 15, 1, 3, 4, 12):
            zz, yy = plus(z, k // 4), plus(y, k % 4)
            remote(ref, ref, s_send.at[2 + m], s_recv.at[2 + m], {"z": zz, "y": yy}).start()

    def directions(m):
        remote(R.at[m], R.at[m], s_send.at[2 + m], s_recv.at[2 + m], partner).wait_recv()
        ref = Dr.at[m, :, c]
        remote(ref, ref, d_send.at[2 + m], d_recv.at[2 + m], partner).start()

    def expand(m):
        ref = Dr.at[m, :, other]
        remote(ref, ref, d_send.at[2 + m], d_recv.at[2 + m], partner).wait_recv()
        direction = Dr[m].reshape(512, 512)
        total = jnp.zeros((8, 512), F32)
        for r in range(4):
            f = F[m, 8 * r : 8 * r + 8].reshape(512, 512)
            e = jnp.dot(f, direction, preferred_element_type=F32)
            E[m, 8 * r : 8 * r + 8] = e.reshape(8, 64, 512)
            total = total + jnp.sum((e * e).reshape(64, 8, 512), axis=0)
        part = total[:, :128] + total[:, 128:256] + total[:, 256:384] + total[:, 384:]
        XR[m, x] = part
        ref = XR.at[m, x]
        for p in xpeers:
            remote(ref, ref, x_send.at[m], x_recv.at[m], p).start()

    def squares(m):
        ref = XR.at[m, pl.ds(0, 3)]
        remote(ref, ref, x_send.at[m], x_recv.at[m], partner).wait_recv()
        ss[m] = (XR[m, 0] + XR[m, 1]) + (XR[m, 2] + XR[m, 3])

    transpose_cols(0)
    fin[0].wait()
    fin[1].wait()
    grad_chunk(0, 0)
    pl.semaphore_wait(bar, 19)
    gather_step(0, 0)
    gather_step(1, 0)
    for m in range(2):
        win[m].wait()
        W[m, me] = wf[m].astype(BF)
    grad_chunk(0, 1)
    grad_chunk(0, 2)
    gather_step(0, 1)
    gather_step(1, 1)
    grad_chunk(0, 3)
    transpose_cols(1)
    grad_chunk(1, 0)
    gather_step(0, 2)
    gather_step(1, 2)
    grad_chunk(1, 1)
    grad_chunk(1, 2)
    gather_step(0, 3)
    gather_step(1, 3)
    grad_chunk(1, 3)
    gather_step(0, 4)
    gather_step(1, 4)
    gather_step(0, 5)
    project(0)
    gather_step(1, 5)
    project(1)
    scatter(0)
    gather_step(2, 0)
    gather_step(3, 0)
    scatter(1)
    for cp in min_:
        cp.wait()
    gather_step(2, 1)
    gather_step(3, 1)
    moments(0)
    gather_step(2, 2)
    gather_step(3, 2)
    moments(1)
    gather_step(2, 3)
    gather_step(3, 3)
    directions(0)
    gather_step(2, 4)
    gather_step(3, 4)
    expand(0)
    directions(1)
    expand(1)
    gather_step(2, 5)
    gather_step(3, 5)
    squares(0)
    squares(1)

    for p in range(4):
        gather_sent(p)
    for m in range(2):
        remote(X.at[m], X.at[m], d_send.at[m], d_recv.at[m], partner).wait_send()
        remote(X.at[m], X.at[m], d_send.at[2 + m], d_recv.at[2 + m], partner).wait_send()
        remote(R.at[m], R.at[m], s_send.at[m], s_recv.at[m], partner).wait_send()
        remote(R.at[m], R.at[m], s_send.at[2 + m], s_recv.at[2 + m], partner).wait_send()
        ref = XR.at[m, pl.ds(0, 3)]
        remote(ref, ref, x_send.at[m], x_recv.at[m], partner).wait_send()


def finish_kernel(
    E, W, mom, ss, w0, w1,
    step0, upd0, fn0, sn0, copy0, step1, upd1, fn1, sn1, copy1,
    wf, stage, st, up, in_sem, sem,
):
    me = (lax.axis_index("z") * 4 + lax.axis_index("y")) * 2 + lax.axis_index("c")
    win = [pltpu.make_async_copy(w, wf.at[m], in_sem.at[m]) for m, w in enumerate((w0, w1))]
    for cp in win:
        cp.start()
    done = []

    def out(src, dst):
        cp = pltpu.make_async_copy(src, dst, sem.at[len(done)])
        cp.start()
        done.append(cp)

    for m, (fn, sn) in enumerate(((fn0, sn0), (fn1, sn1))):
        out(mom.at[m, 0], fn)
        out(mom.at[m, 1], sn)
    for m, (step, upd, copy) in enumerate(((step0, upd0, copy0), (step1, upd1, copy1))):
        mean_square = jnp.sum(ss[m]) / (D * HV)
        scale = step_rate / jnp.sqrt(jnp.full((8, 512), mean_square, F32) + scale_floor)
        for r in range(4):
            e = E[m, 8 * r : 8 * r + 8].reshape(64, 8, 512)
            w = W[m, 8 * r : 8 * r + 8].reshape(512, 512).astype(F32)
            new = w - (scale[None] * e).reshape(512, 512)
            stage[m, 512 * r : 512 * r + 512] = new.astype(BF)
            out(stage.at[m, pl.ds(512 * r, 512)], copy.at[pl.ds(512 * r, 512)])
        win[m].wait()
        own = (scale[None] * E[m, me].reshape(8, 8, 512)).reshape(64, 512)
        st[m] = own
        up[m] = wf[m] - own
        out(st.at[m], step)
        out(up.at[m], upd)
    for cp in done:
        cp.wait()


def local(
    model_input, value_cotan, mixer_cotan, head_output,
    value_weight, value_factor, value_first, value_second,
    output_weight, output_factor, output_first, output_second,
):
    any_spec = pl.BlockSpec(memory_space=pl.ANY)
    vmem_spec = pl.BlockSpec(memory_space=pltpu.VMEM)
    DMA = pltpu.SemaphoreType.DMA
    E, W, mom, ss = pl.pallas_call(
        exchange_kernel,
        out_shape=(
            pltpu.VMEM((2, 32, 64, 512), F32),
            pltpu.VMEM((2, 32, 64, 512), BF),
            pltpu.VMEM((2, 2, 16, 512), F32),
            pltpu.VMEM((2, 8, 128), F32),
        ),
        in_specs=[any_spec] * 12,
        out_specs=(vmem_spec,) * 4,
        scratch_shapes=[
            pltpu.VMEM((2, 4, 2048, 512), BF),
            pltpu.VMEM((2, 2048, 512), BF),
            pltpu.VMEM((2, 512, 2048), BF),
            pltpu.VMEM((2, 512, 2048), BF),
            pltpu.VMEM((2, 32, 64, 512), BF),
            pltpu.VMEM((2, 64, 512), F32),
            pltpu.VMEM((4, 16, 512), F32),
            pltpu.VMEM((2, 16, 2, 16, 512), BF),
            pltpu.VMEM((2, 16, 16, 512), BF),
            pltpu.VMEM((2, 16, 16, 512), BF),
            pltpu.VMEM((2, 15, 16, 512), BF),
            pltpu.VMEM((2, 16, 2, 16, 512), BF),
            pltpu.VMEM((2, 4, 8, 128), F32),
            DMA((18,)),
            DMA((4,)),
            DMA((4, 11)),
            DMA((4,)),
            DMA((4,)),
            DMA((4,)),
            DMA((4,)),
            DMA((2,)),
            DMA((2,)),
        ],
        compiler_params=pltpu.CompilerParams(
            collective_id=0, has_side_effects=True, vmem_limit_bytes=44 * 1024 * 1024
        ),
        name="exchange",
    )(
        model_input, value_cotan, mixer_cotan, head_output,
        value_weight, output_weight, value_factor, output_factor,
        value_first, value_second, output_first, output_second,
    )
    shapes = []
    for _ in range(2):
        shapes += [
            jax.ShapeDtypeStruct((64, 512), F32),
            jax.ShapeDtypeStruct((64, 512), F32),
            jax.ShapeDtypeStruct((16, 512), F32),
            jax.ShapeDtypeStruct((16, 512), F32),
            jax.ShapeDtypeStruct((2048, 512), BF),
        ]
    return pl.pallas_call(
        finish_kernel,
        out_shape=tuple(shapes),
        in_specs=[vmem_spec] * 4 + [any_spec] * 2,
        out_specs=(any_spec,) * 10,
        scratch_shapes=[
            pltpu.VMEM((2, 64, 512), F32),
            pltpu.VMEM((2, 2048, 512), BF),
            pltpu.VMEM((2, 64, 512), F32),
            pltpu.VMEM((2, 64, 512), F32),
            DMA((2,)),
            DMA((16,)),
        ],
        compiler_params=pltpu.CompilerParams(vmem_limit_bytes=16 * 1024 * 1024),
        name="finish",
    )(E, W, mom, ss, value_weight, output_weight)


def solution(mesh):
    torus = Mesh(mesh.devices.reshape(4, 4, 2, mesh.shape["tp"]), ("z", "y", "c", "x"))
    rows, cols = P(FS, None), P(FS, "x")
    part = (cols, cols, cols, cols, P(None, "x"))
    return jax.shard_map(
        local, mesh=torus,
        in_specs=(rows, cols, rows, cols, cols, rows, cols, cols, cols, rows, cols, cols),
        out_specs=part + part, check_vma=False,
    )
```

```python
import functools

import jax
import jax.numpy as jnp
from jax import lax
from jax.experimental import pallas as pl
from jax.experimental.pallas import tpu as pltpu
from jax.sharding import Mesh
from jax.sharding import PartitionSpec as P

D = 2048
HV = 2048
FS = ("z", "y", "c")
MESH = pl.DeviceIdType.MESH

beta_first = 0.8
beta_second = 0.9
step_rate = 0.02
scale_floor = 0.25
tiny_eps = 1e-08

BF = jnp.bfloat16
F32 = jnp.float32


def exchange_kernel(
    rows0, cols0, rows1, cols1, w0, w1, f0, f1, a0, b0, a1, b1,
    E, W, mom, ss,
    rows, cols, colsT, gT, F, wf, mo, Pj, X, S, R, Dr, XR,
    in_sem, g_send, g_recv, d_send, d_recv, s_send, s_recv, x_send, x_recv,
):
    z, y, c, x = (lax.axis_index(n) for n in ("z", "y", "c", "x"))
    chip = z * 4 + y
    other = 1 - c
    ra = y + c * (z - y)
    rb = z + c * (y - z)

    def place(a, b):
        zz = b + c * (a - b)
        yy = a + c * (b - a)
        return zz, yy

    def shard(a, b):
        zz, yy = place(a, b)
        return (zz * 4 + yy) * 2 + c

    def at(a, b):
        zz, yy = place(a, b)
        return {"z": zz, "y": yy}

    def plus(v, k):
        return lax.rem(v + k, 4)

    def remote(src, dst, ssem, rsem, dev):
        return pltpu.make_async_remote_copy(
            src_ref=src, dst_ref=dst, send_sem=ssem, recv_sem=rsem,
            device_id=dev, device_id_type=MESH,
        )

    partner = {"c": other}

    bar = pltpu.get_barrier_semaphore()
    peers = [{"z": plus(z, k)} for k in range(1, 4)] + [{"y": plus(y, k)} for k in range(1, 4)]
    xpeers = [{"x": plus(x, k)} for k in range(1, 4)]
    for p in peers + [partner] + xpeers:
        pl.semaphore_signal(bar, inc=1, device_id=p, device_id_type=MESH)

    me = chip * 2 + c
    fin = [pltpu.make_async_copy(f, F.at[m, me], in_sem.at[m]) for m, f in enumerate((f0, f1))]
    win = [pltpu.make_async_copy(w, wf.at[m], in_sem.at[2 + m]) for m, w in enumerate((w0, w1))]
    cin = [pltpu.make_async_copy(v, cols.at[m], in_sem.at[4 + m]) for m, v in enumerate((cols0, cols1))]
    rin = [
        [
            pltpu.make_async_copy(
                v.at[:, pl.ds(512 * j, 512)], rows.at[m, j], in_sem.at[6 + 4 * m + j]
            )
            for j in range(4)
        ]
        for m, v in enumerate((rows0, rows1))
    ]
    min_ = [
        pltpu.make_async_copy(v, mo.at[i], in_sem.at[14 + i]) for i, v in enumerate((a0, b0, a1, b1))
    ]
    for cp in fin + [cin[0]] + win + rin[0] + [cin[1]] + rin[1] + min_:
        cp.start()

    def G(p):
        return W.at[p - 2]

    am, ap, af = plus(ra, 3), plus(ra, 1), plus(ra, 2)
    bm, bp, bf = plus(rb, 3), plus(rb, 1), plus(rb, 2)
    LO, HI = pl.ds(0, 32), pl.ds(32, 32)

    def send(p, s, dev, k, half=None):
        ref = G(p).at[s] if half is None else G(p).at[s, half]
        remote(ref, ref, g_send.at[p], g_recv.at[p, k], dev).start()

    def arrived(p, k, n):
        ref = G(p).at[pl.ds(0, n)]
        remote(ref, ref, g_send.at[p], g_recv.at[p, k], partner).wait_recv()

    def across(p, s):
        send(p, s, partner, 10)

    def gather_step(p, step):
        if step == 0:
            s = shard(ra, rb)
            send(p, s, at(ap, rb), 0)
            send(p, s, at(am, rb), 1)
            send(p, s, at(ra, bp), 3)
            send(p, s, at(ra, bm), 4)
            across(p, s)
        if step == 1:
            arrived(p, 0, 1)
            send(p, shard(am, rb), at(ap, rb), 2, LO)
            arrived(p, 1, 1)
            send(p, shard(ap, rb), at(am, rb), 2, HI)
            for a in (am, ap):
                send(p, shard(a, rb), at(ra, bp), 5)
                send(p, shard(a, rb), at(ra, bm), 6)
            arrived(p, 3, 1)
            send(p, shard(ra, bm), at(ra, bp), 9, LO)
            arrived(p, 4, 1)
            send(p, shard(ra, bp), at(ra, bm), 9, HI)
            for s in (shard(am, rb), shard(ap, rb), shard(ra, bm), shard(ra, bp)):
                across(p, s)
        if step == 2:
            arrived(p, 2, 1)
            send(p, shard(af, rb), at(ra, bp), 7)
            send(p, shard(af, rb), at(ra, bm), 8)
            arrived(p, 5, 2)
            for a in (am, ap):
                send(p, shard(a, bm), at(ra, bp), 9, LO)
            arrived(p, 6, 2)
            for a in (am, ap):
                send(p, shard(a, bp), at(ra, bm), 9, HI)
            across(p, shard(af, rb))
            for a in (am, ap):
                across(p, shard(a, bm))
                across(p, shard(a, bp))
        if step == 3:
            arrived(p, 7, 1)
            send(p, shard(af, bm), at(ra, bp), 9, LO)
            arrived(p, 8, 1)
            send(p, shard(af, bp), at(ra, bm), 9, HI)
            across(p, shard(af, bm))
            across(p, shard(af, bp))
        if step == 4:
            arrived(p, 9, 4)
            for a in (ra, am, ap, af):
                across(p, shard(a, bf))
        if step == 5:
            arrived(p, 10, 16)

    mine = pl.ds(32 * lax.rem(x, 2), 32)
    xp, xm = {"x": plus(x, 1)}, {"x": plus(x, 3)}

    def send_half(p, s, dev, k):
        ref = F.at[p, s, mine]
        remote(ref, ref, g_send.at[p], g_recv.at[p, k], dev).start()

    def halves(p, k, n):
        ref = F.at[p, pl.ds(0, n), pl.ds(0, 32)]
        remote(ref, ref, g_send.at[p], g_recv.at[p, k], partner).wait_recv()

    theirs = pl.ds(32 - 32 * lax.rem(x, 2), 32)

    def over(p, s, part=None):
        ref = F.at[p, s] if part is None else F.at[p, s, part]
        remote(ref, ref, g_send.at[4 + p], g_recv.at[p, 10], partner).start()

    def half_step(p, step):
        if step == 0:
            s = shard(ra, rb)
            for k, a in ((2, af), (0, ap), (1, am)):
                send_half(p, s, at(a, rb), k)
            for k, b in ((5, bf), (3, bp), (4, bm)):
                send_half(p, s, at(ra, b), k)
            over(p, s)
        if step == 1:
            for k, a, dev, q in ((0, am, xp, 11), (1, ap, xm, 12), (2, af, xp, 11)):
                halves(p, k, 1)
                s = shard(a, rb)
                for r, b in ((8, bf), (6, bp), (7, bm)):
                    send_half(p, s, at(ra, b), r)
                send_half(p, s, dev, q)
                over(p, s, mine)
            for k, b, dev, q in ((3, bm, xm, 12), (4, bp, xp, 11), (5, bf, xm, 12)):
                halves(p, k, 1)
                send_half(p, shard(ra, b), dev, q)
                over(p, shard(ra, b), mine)
        if step == 2:
            for k, b, f in ((6, bm, 0), (7, bp, 1), (8, bf, 0)):
                halves(p, k, 3)
                for n, a in enumerate((am, ap, af)):
                    if (n + f) % 2:
                        send_half(p, shard(a, b), xp, 13)
                    else:
                        send_half(p, shard(a, b), xm, 14)
                    over(p, shard(a, b), mine)
        if step == 3:
            halves(p, 11, 3)
            for s in (shard(am, rb), shard(af, rb), shard(ra, bp)):
                over(p, s, theirs)
            halves(p, 12, 3)
            for s in (shard(ap, rb), shard(ra, bm), shard(ra, bf)):
                over(p, s, theirs)
        if step == 4:
            halves(p, 13, 4)
            for s in (shard(ap, bm), shard(am, bp), shard(af, bp), shard(ap, bf)):
                over(p, s, theirs)
            halves(p, 14, 5)
            for s in (shard(am, bm), shard(af, bm), shard(ap, bp), shard(am, bf), shard(af, bf)):
                over(p, s, theirs)
        if step == 5:
            ref = F.at[p, pl.ds(0, 16)]
            remote(ref, ref, g_send.at[4 + p], g_recv.at[p, 10], partner).wait_recv()

    def gather_sent(p):
        ref = G(p).at[pl.ds(0, 31)]
        remote(ref, ref, g_send.at[p], g_recv.at[p, 0], partner).wait_send()

    def round_weights():
        for m in range(2):
            win[m].wait()
            W[m, me] = wf[m].astype(BF)

    def transpose_cols(m):
        cin[m].wait()
        for t in range(4):
            colsT[m, :, 512 * t : 512 * t + 512] = cols[m, 512 * t : 512 * t + 512, :].T

    def grad_chunk(m, j):
        rin[m][j].wait()
        out = jnp.dot(colsT[m], rows[m, j], preferred_element_type=F32)
        gT[m, :, 512 * j : 512 * j + 512] = out.astype(BF)

    def to_partner(m):
        return remote(Pj.at[m, :, other], X.at[m], d_send.at[m], d_recv.at[m], partner)

    def project(m):
        for n in range(2):
            f = F[m, :, :, 256 * n : 256 * n + 256].reshape(D, 256)
            out = jnp.dot(gT[m], f, preferred_element_type=F32)
            Pj[m, 8 * n : 8 * n + 8] = out.T.astype(BF).reshape(8, 2, 16, 512)
        to_partner(m).start()

    FAR_FIRST = (10, 9, 11, 6, 14, 2, 8, 5, 7, 13, 15, 1, 3, 4, 12)

    def scatter(m):
        to_partner(m).wait_recv()
        S[m] = (Pj[m, :, c].astype(F32) + X[m].astype(F32)).astype(BF)
        for k in FAR_FIRST:
            zz, yy = plus(z, k // 4), plus(y, k % 4)
            remote(
                S.at[m, zz * 4 + yy], R.at[m, k - 1], s_send.at[m], s_recv.at[m],
                {"z": zz, "y": yy},
            ).start()

    def moments(m):
        for cp in min_[2 * m : 2 * m + 2]:
            cp.wait()
        remote(R.at[m], R.at[m], s_send.at[m], s_recv.at[m], partner).wait_recv()
        proj = S[m, chip].astype(F32) + jnp.sum(R[m].astype(F32), axis=0)
        fnew = beta_first * mo[2 * m] + (1.0 - beta_first) * proj
        snew = beta_second * mo[2 * m + 1] + (1.0 - beta_second) * proj * proj
        mom[m, 0] = fnew
        mom[m, 1] = snew
        Dr[m, chip, c] = (fnew / (jnp.sqrt(snew) + tiny_eps)).astype(BF)
        ref = Dr.at[m, chip, c]
        for k in FAR_FIRST:
            zz, yy = plus(z, k // 4), plus(y, k % 4)
            remote(ref, ref, s_send.at[2 + m], s_recv.at[2 + m], {"z": zz, "y": yy}).start()

    def directions(m):
        remote(R.at[m], R.at[m], s_send.at[2 + m], s_recv.at[2 + m], partner).wait_recv()
        ref = Dr.at[m, :, c]
        remote(ref, ref, d_send.at[2 + m], d_recv.at[2 + m], partner).start()

    def expand(m):
        ref = Dr.at[m, :, other]
        remote(ref, ref, d_send.at[2 + m], d_recv.at[2 + m], partner).wait_recv()
        direction = Dr[m].reshape(512, 512)
        total = jnp.zeros((8, 512), F32)
        for r in range(4):
            f = F[m, 8 * r : 8 * r + 8].reshape(512, 512)
            e = jnp.dot(f, direction, preferred_element_type=F32)
            E[m, 8 * r : 8 * r + 8] = e.reshape(8, 64, 512)
            total = total + jnp.sum((e * e).reshape(64, 8, 512), axis=0)
        part = total[:, :128] + total[:, 128:256] + total[:, 256:384] + total[:, 384:]
        XR[m, x] = part
        ref = XR.at[m, x]
        for p in xpeers:
            remote(ref, ref, x_send.at[m], x_recv.at[m], p).start()

    def squares(m):
        ref = XR.at[m, pl.ds(0, 3)]
        remote(ref, ref, x_send.at[m], x_recv.at[m], partner).wait_recv()
        ss[m] = (XR[m, 0] + XR[m, 1]) + (XR[m, 2] + XR[m, 3])

    fin[0].wait()
    fin[1].wait()
    pl.semaphore_wait(bar, 10)
    half_step(0, 0)
    half_step(1, 0)
    round_weights()
    gather_step(2, 0)
    transpose_cols(0)
    grad_chunk(0, 0)
    grad_chunk(0, 1)
    half_step(0, 1)
    grad_chunk(0, 2)
    half_step(1, 1)
    gather_step(3, 0)
    grad_chunk(0, 3)
    gather_step(2, 1)
    transpose_cols(1)
    grad_chunk(1, 0)
    half_step(0, 2)
    grad_chunk(1, 1)
    half_step(1, 2)
    grad_chunk(1, 2)
    half_step(0, 3)
    gather_step(3, 1)
    grad_chunk(1, 3)
    half_step(0, 4)
    gather_step(2, 2)
    half_step(0, 5)
    project(0)
    half_step(1, 3)
    half_step(1, 4)
    gather_step(3, 2)
    scatter(0)
    half_step(1, 5)
    project(1)
    gather_step(2, 3)
    gather_step(3, 3)
    scatter(1)
    moments(0)
    moments(1)
    gather_step(2, 4)
    gather_step(3, 4)
    directions(0)
    directions(1)
    expand(0)
    expand(1)
    gather_step(2, 5)
    gather_step(3, 5)
    squares(0)
    squares(1)

    for p in range(2):
        gather_sent(2 + p)
        ref = F.at[p, pl.ds(0, 30), pl.ds(0, 32)]
        remote(ref, ref, g_send.at[p], g_recv.at[p, 0], partner).wait_send()
        ref = F.at[p, pl.ds(0, 16)]
        remote(ref, ref, g_send.at[4 + p], g_recv.at[p, 0], partner).wait_send()
    for m in range(2):
        to_partner(m).wait_send()
        remote(X.at[m], X.at[m], d_send.at[2 + m], d_recv.at[2 + m], partner).wait_send()
        remote(R.at[m], R.at[m], s_send.at[m], s_recv.at[m], partner).wait_send()
        remote(R.at[m], R.at[m], s_send.at[2 + m], s_recv.at[2 + m], partner).wait_send()
        ref = XR.at[m, pl.ds(0, 3)]
        remote(ref, ref, x_send.at[m], x_recv.at[m], partner).wait_send()


def finish_kernel(
    E, W, mom, ss, w0, w1,
    step0, upd0, fn0, sn0, copy0, step1, upd1, fn1, sn1, copy1,
    wf, stage, st, up, in_sem, sem,
):
    me = (lax.axis_index("z") * 4 + lax.axis_index("y")) * 2 + lax.axis_index("c")
    win = [pltpu.make_async_copy(w, wf.at[m], in_sem.at[m]) for m, w in enumerate((w0, w1))]
    for cp in win:
        cp.start()
    done = []

    def out(src, dst):
        cp = pltpu.make_async_copy(src, dst, sem.at[len(done)])
        cp.start()
        done.append(cp)

    for m, (fn, sn) in enumerate(((fn0, sn0), (fn1, sn1))):
        out(mom.at[m, 0], fn)
        out(mom.at[m, 1], sn)
    for m, (step, upd, copy) in enumerate(((step0, upd0, copy0), (step1, upd1, copy1))):
        mean_square = jnp.sum(ss[m]) / (D * HV)
        scale = step_rate / jnp.sqrt(jnp.full((8, 512), mean_square, F32) + scale_floor)
        for r in range(8):
            e = E[m, 4 * r : 4 * r + 4].reshape(32, 8, 512)
            w = W[m, 4 * r : 4 * r + 4].reshape(256, 512).astype(F32)
            new = w - (scale[None] * e).reshape(256, 512)
            stage[m, 256 * r : 256 * r + 256] = new.astype(BF)
            out(stage.at[m, pl.ds(256 * r, 256)], copy.at[pl.ds(256 * r, 256)])
        win[m].wait()
        own = (scale[None] * E[m, me].reshape(8, 8, 512)).reshape(64, 512)
        st[m] = own
        up[m] = wf[m] - own
        out(st.at[m], step)
        out(up.at[m], upd)
    for cp in done:
        cp.wait()


def local(
    model_input, value_cotan, mixer_cotan, head_output,
    value_weight, value_factor, value_first, value_second,
    output_weight, output_factor, output_first, output_second,
):
    any_spec = pl.BlockSpec(memory_space=pl.ANY)
    vmem_spec = pl.BlockSpec(memory_space=pltpu.VMEM)
    DMA = pltpu.SemaphoreType.DMA
    E, W, mom, ss = pl.pallas_call(
        exchange_kernel,
        out_shape=(
            pltpu.VMEM((2, 32, 64, 512), F32),
            pltpu.VMEM((2, 32, 64, 512), BF),
            pltpu.VMEM((2, 2, 16, 512), F32),
            pltpu.VMEM((2, 8, 128), F32),
        ),
        in_specs=[any_spec] * 12,
        out_specs=(vmem_spec,) * 4,
        scratch_shapes=[
            pltpu.VMEM((2, 4, 2048, 512), BF),
            pltpu.VMEM((2, 2048, 512), BF),
            pltpu.VMEM((2, 512, 2048), BF),
            pltpu.VMEM((2, 512, 2048), BF),
            pltpu.VMEM((2, 32, 64, 512), BF),
            pltpu.VMEM((2, 64, 512), F32),
            pltpu.VMEM((4, 16, 512), F32),
            pltpu.VMEM((2, 16, 2, 16, 512), BF),
            pltpu.VMEM((2, 16, 16, 512), BF),
            pltpu.VMEM((2, 16, 16, 512), BF),
            pltpu.VMEM((2, 15, 16, 512), BF),
            pltpu.VMEM((2, 16, 2, 16, 512), BF),
            pltpu.VMEM((2, 4, 8, 128), F32),
            DMA((18,)),
            DMA((6,)),
            DMA((4, 15)),
            DMA((4,)),
            DMA((4,)),
            DMA((4,)),
            DMA((4,)),
            DMA((2,)),
            DMA((2,)),
        ],
        compiler_params=pltpu.CompilerParams(
            collective_id=0, has_side_effects=True, vmem_limit_bytes=44 * 1024 * 1024
        ),
        name="exchange",
    )(
        model_input, value_cotan, mixer_cotan, head_output,
        value_weight, output_weight, value_factor, output_factor,
        value_first, value_second, output_first, output_second,
    )
    shapes = []
    for _ in range(2):
        shapes += [
            jax.ShapeDtypeStruct((64, 512), F32),
            jax.ShapeDtypeStruct((64, 512), F32),
            jax.ShapeDtypeStruct((16, 512), F32),
            jax.ShapeDtypeStruct((16, 512), F32),
            jax.ShapeDtypeStruct((2048, 512), BF),
        ]
    return pl.pallas_call(
        finish_kernel,
        out_shape=tuple(shapes),
        in_specs=[vmem_spec] * 4 + [any_spec] * 2,
        out_specs=(any_spec,) * 10,
        scratch_shapes=[
            pltpu.VMEM((2, 64, 512), F32),
            pltpu.VMEM((2, 2048, 512), BF),
            pltpu.VMEM((2, 64, 512), F32),
            pltpu.VMEM((2, 64, 512), F32),
            DMA((2,)),
            DMA((24,)),
        ],
        compiler_params=pltpu.CompilerParams(vmem_limit_bytes=16 * 1024 * 1024),
        name="finish",
    )(E, W, mom, ss, value_weight, output_weight)


def solution(mesh):
    torus = Mesh(mesh.devices.reshape(4, 4, 2, mesh.shape["tp"]), ("z", "y", "c", "x"))
    rows, cols = P(FS, None), P(FS, "x")
    part = (cols, cols, cols, cols, P(None, "x"))
    return jax.shard_map(
        local, mesh=torus,
        in_specs=(rows, cols, rows, cols, cols, rows, cols, cols, cols, rows, cols, cols),
        out_specs=part + part, check_vma=False,
    )
```

```python
import functools

import jax
import jax.numpy as jnp
from jax import lax
from jax.experimental import pallas as pl
from jax.experimental.pallas import tpu as pltpu
from jax.sharding import Mesh
from jax.sharding import PartitionSpec as P

D = 2048
HV = 2048
FS = ("z", "y", "c")
MESH = pl.DeviceIdType.MESH

beta_first = 0.8
beta_second = 0.9
step_rate = 0.02
scale_floor = 0.25
tiny_eps = 1e-08

BF = jnp.bfloat16
F32 = jnp.float32


def scale_of(squares):
    mean_square = jnp.sum(squares) / (D * HV)
    return step_rate / jnp.sqrt(jnp.full((8, 512), mean_square, F32) + scale_floor)


def new_step(scale, expanded):
    return (scale[None] * expanded.reshape(-1, 8, 512)).reshape(-1, 512)


def new_copy(scale, expanded, weight):
    return (weight.reshape(-1, 512).astype(F32) - new_step(scale, expanded)).astype(BF)


def exchange_kernel(
    rows0, cols0, rows1, cols1, w0, w1, f0, f1, a0, b0, a1, b1,
    E1, W, mom, ss, copy, own,
    E0, rows, cols, colsT, gT, F, wf, mo, Pj, X, S, R, Dr, XR,
    in_sem, g_send, g_recv, d_send, d_recv, s_send, s_recv, x_send, x_recv,
):
    z, y, c, x = (lax.axis_index(n) for n in ("z", "y", "c", "x"))
    chip = z * 4 + y
    other = 1 - c
    ra = y + c * (z - y)
    rb = z + c * (y - z)

    def place(a, b):
        zz = b + c * (a - b)
        yy = a + c * (b - a)
        return zz, yy

    def shard(a, b):
        zz, yy = place(a, b)
        return (zz * 4 + yy) * 2 + c

    def at(a, b):
        zz, yy = place(a, b)
        return {"z": zz, "y": yy}

    def plus(v, k):
        return lax.rem(v + k, 4)

    def remote(src, dst, ssem, rsem, dev):
        return pltpu.make_async_remote_copy(
            src_ref=src, dst_ref=dst, send_sem=ssem, recv_sem=rsem,
            device_id=dev, device_id_type=MESH,
        )

    partner = {"c": other}

    bar = pltpu.get_barrier_semaphore()
    peers = [{"z": plus(z, k)} for k in range(1, 4)] + [{"y": plus(y, k)} for k in range(1, 4)]
    xpeers = [{"x": plus(x, k)} for k in range(1, 4)]
    for p in peers + [partner] + xpeers:
        pl.semaphore_signal(bar, inc=1, device_id=p, device_id_type=MESH)

    me = chip * 2 + c
    fin = [pltpu.make_async_copy(f, F.at[m, me], in_sem.at[0]) for m, f in enumerate((f0, f1))]
    win = [pltpu.make_async_copy(w, wf.at[m], in_sem.at[1]) for m, w in enumerate((w0, w1))]
    cin = [pltpu.make_async_copy(v, cols.at[m], in_sem.at[2 + m]) for m, v in enumerate((cols0, cols1))]
    rin = [
        [
            pltpu.make_async_copy(
                v.at[:, pl.ds(512 * j, 512)], rows.at[m, j], in_sem.at[4 + 4 * m + j]
            )
            for j in range(4)
        ]
        for m, v in enumerate((rows0, rows1))
    ]
    min_ = [
        pltpu.make_async_copy(v, mo.at[i], in_sem.at[12]) for i, v in enumerate((a0, b0, a1, b1))
    ]
    for cp in fin + [cin[0]] + win + rin[0] + [cin[1]] + rin[1] + min_:
        cp.start()

    def loaded(ref, k):
        pltpu.make_async_copy(ref, ref, in_sem.at[k]).wait()

    def G(p):
        return W.at[p - 2]

    am, ap, af = plus(ra, 3), plus(ra, 1), plus(ra, 2)
    bm, bp, bf = plus(rb, 3), plus(rb, 1), plus(rb, 2)
    LO, HI = pl.ds(0, 32), pl.ds(32, 32)

    def send(p, s, dev, k, half=None):
        ref = G(p).at[s] if half is None else G(p).at[s, half]
        remote(ref, ref, g_send.at[1], g_recv.at[6 + 7 * p + k], dev).start()

    def arrived(p, k, n):
        ref = G(p).at[pl.ds(0, n)]
        remote(ref, ref, g_send.at[1], g_recv.at[6 + 7 * p + k], partner).wait_recv()

    def across(p, s):
        send(p, s, partner, 6)

    def gather_step(p, step):
        if step == 0:
            s = shard(ra, rb)
            send(p, s, at(ap, rb), 0)
            send(p, s, at(am, rb), 0)
            send(p, s, at(ra, bp), 2)
            send(p, s, at(ra, bm), 2)
            across(p, s)
        if step == 1:
            arrived(p, 0, 2)
            send(p, shard(am, rb), at(ap, rb), 1, LO)
            send(p, shard(ap, rb), at(am, rb), 1, HI)
            for a in (am, ap):
                send(p, shard(a, rb), at(ra, bp), 3)
                send(p, shard(a, rb), at(ra, bm), 3)
            arrived(p, 2, 2)
            send(p, shard(ra, bm), at(ra, bp), 5, LO)
            send(p, shard(ra, bp), at(ra, bm), 5, HI)
            for s in (shard(am, rb), shard(ap, rb), shard(ra, bm), shard(ra, bp)):
                across(p, s)
        if step == 2:
            arrived(p, 1, 1)
            send(p, shard(af, rb), at(ra, bp), 4)
            send(p, shard(af, rb), at(ra, bm), 4)
            arrived(p, 3, 4)
            for a in (am, ap):
                send(p, shard(a, bm), at(ra, bp), 5, LO)
                send(p, shard(a, bp), at(ra, bm), 5, HI)
            across(p, shard(af, rb))
            for a in (am, ap):
                across(p, shard(a, bm))
                across(p, shard(a, bp))
        if step == 3:
            arrived(p, 4, 2)
            send(p, shard(af, bm), at(ra, bp), 5, LO)
            send(p, shard(af, bp), at(ra, bm), 5, HI)
            across(p, shard(af, bm))
            across(p, shard(af, bp))
        if step == 4:
            arrived(p, 5, 4)
            for a in (ra, am, ap, af):
                across(p, shard(a, bf))
        if step == 5:
            arrived(p, 6, 16)

    mine = pl.ds(32 * lax.rem(x, 2), 32)
    xp, xm = {"x": plus(x, 1)}, {"x": plus(x, 3)}

    theirs = pl.ds(32 - 32 * lax.rem(x, 2), 32)

    def send_half(p, s, dev, k):
        ref = F.at[p, s, mine]
        remote(ref, ref, g_send.at[0], g_recv.at[10 * p + k], dev).start()

    def halves(p, k, n):
        ref = F.at[p, pl.ds(0, n), pl.ds(0, 32)]
        remote(ref, ref, g_send.at[0], g_recv.at[10 * p + k], partner).wait_recv()

    def over(p, s, part=None):
        ref = F.at[p, s] if part is None else F.at[p, s, part]
        remote(ref, ref, g_send.at[0], g_recv.at[10 * p + 7], partner).start()

    def half_step(p, step):
        if step == 0:
            s = shard(ra, rb)
            for k, a in ((2, af), (0, ap), (1, am)):
                send_half(p, s, at(a, rb), k)
            for b in (bf, bp, bm):
                send_half(p, s, at(ra, b), 3)
            over(p, s)
        if step == 1:
            for k, a, dev in ((0, am, xp), (1, ap, xm), (2, af, xp)):
                halves(p, k, 1)
                s = shard(a, rb)
                for q, b in ((6, bf), (4, bp), (5, bm)):
                    send_half(p, s, at(ra, b), q)
                send_half(p, s, dev, 8)
                over(p, s, mine)
            halves(p, 3, 3)
            for b, dev in ((bm, xm), (bp, xp), (bf, xm)):
                send_half(p, shard(ra, b), dev, 8)
                over(p, shard(ra, b), mine)
        if step == 2:
            for k, b, f in ((4, bm, 0), (5, bp, 1), (6, bf, 0)):
                halves(p, k, 3)
                for n, a in enumerate((am, ap, af)):
                    send_half(p, shard(a, b), xp if (n + f) % 2 else xm, 9)
                    over(p, shard(a, b), mine)
        if step == 3:
            halves(p, 8, 6)
            for s in [shard(a, rb) for a in (am, ap, af)] + [shard(ra, b) for b in (bm, bp, bf)]:
                over(p, s, theirs)
        if step == 4:
            halves(p, 9, 9)
            for b in (bm, bp, bf):
                for a in (am, ap, af):
                    over(p, shard(a, b), theirs)
        if step == 5:
            ref = F.at[p, pl.ds(0, 16)]
            remote(ref, ref, g_send.at[0], g_recv.at[10 * p + 7], partner).wait_recv()

    def all_sent(array, k):
        ref = array.at[:, pl.ds(0, 31)]
        remote(ref, ref, g_send.at[k], g_recv.at[0], partner).wait_send()

    def round_weights():
        loaded(wf, 1)
        for m in range(2):
            W[m, me] = wf[m].astype(BF)

    def transpose_cols(m):
        cin[m].wait()
        for t in range(4):
            colsT[m, :, 512 * t : 512 * t + 512] = cols[m, 512 * t : 512 * t + 512, :].T

    def grad_chunk(m, j):
        rin[m][j].wait()
        out = jnp.dot(colsT[m], rows[m, j], preferred_element_type=F32)
        gT[m, :, 512 * j : 512 * j + 512] = out.astype(BF)

    def to_partner(m):
        return remote(Pj.at[m, :, other], X.at[m], d_send.at[0], d_recv.at[m], partner)

    def project(m):
        for n in range(2):
            f = F[m, :, :, 256 * n : 256 * n + 256].reshape(D, 256)
            out = jnp.dot(gT[m], f, preferred_element_type=F32)
            Pj[m, 8 * n : 8 * n + 8] = out.T.astype(BF).reshape(8, 2, 16, 512)
        to_partner(m).start()

    FAR_FIRST = (10, 9, 11, 6, 14, 2, 8, 5, 7, 13, 15, 1, 3, 4, 12)

    def scatter(m):
        to_partner(m).wait_recv()
        S[m] = (Pj[m, :, c].astype(F32) + X[m].astype(F32)).astype(BF)
        for k in FAR_FIRST:
            zz, yy = plus(z, k // 4), plus(y, k % 4)
            remote(
                S.at[m, zz * 4 + yy], R.at[m, k - 1], s_send.at[0], s_recv.at[m],
                {"z": zz, "y": yy},
            ).start()

    def moments(m):
        if m == 0:
            loaded(mo, 12)
        remote(R.at[m], R.at[m], s_send.at[0], s_recv.at[m], partner).wait_recv()
        proj = S[m, chip].astype(F32) + jnp.sum(R[m].astype(F32), axis=0)
        fnew = beta_first * mo[2 * m] + (1.0 - beta_first) * proj
        snew = beta_second * mo[2 * m + 1] + (1.0 - beta_second) * proj * proj
        mom[m, 0] = fnew
        mom[m, 1] = snew
        Dr[m, chip, c] = (fnew / (jnp.sqrt(snew) + tiny_eps)).astype(BF)
        ref = Dr.at[m, chip, c]
        for k in FAR_FIRST:
            zz, yy = plus(z, k // 4), plus(y, k % 4)
            remote(ref, ref, s_send.at[1], s_recv.at[2 + m], {"z": zz, "y": yy}).start()

    def directions(m):
        remote(R.at[m], R.at[m], s_send.at[1], s_recv.at[2 + m], partner).wait_recv()
        ref = Dr.at[m, :, c]
        remote(ref, ref, d_send.at[1], d_recv.at[2 + m], partner).start()

    def expand(m):
        ref = Dr.at[m, :, other]
        remote(ref, ref, d_send.at[1], d_recv.at[2 + m], partner).wait_recv()
        direction = Dr[m].reshape(512, 512)
        total = jnp.zeros((8, 512), F32)
        for r in range(4):
            f = F[m, 8 * r : 8 * r + 8].reshape(512, 512)
            e = jnp.dot(f, direction, preferred_element_type=F32)
            (E0, E1)[m][8 * r : 8 * r + 8] = e.reshape(8, 64, 512)
            total = total + jnp.sum((e * e).reshape(64, 8, 512), axis=0)
        part = total[:, :128] + total[:, 128:256] + total[:, 256:384] + total[:, 384:]
        XR[m, x] = part
        ref = XR.at[m, x]
        for p in xpeers:
            remote(ref, ref, x_send.at[0], x_recv.at[m], p).start()

    def squares(m):
        ref = XR.at[m, pl.ds(0, 3)]
        remote(ref, ref, x_send.at[0], x_recv.at[m], partner).wait_recv()
        return (XR[m, 0] + XR[m, 1]) + (XR[m, 2] + XR[m, 3])

    def finish_first(total):
        scale = scale_of(total)
        for r in range(8):
            copy[256 * r : 256 * r + 256] = new_copy(scale, E0[4 * r : 4 * r + 4], W[0, 4 * r : 4 * r + 4])
        step = new_step(scale, E0[me])
        own[0] = step
        own[1] = wf[0] - step

    loaded(F.at[:, me], 0)
    pl.semaphore_wait(bar, 10)
    half_step(0, 0)
    half_step(1, 0)
    transpose_cols(0)
    round_weights()
    gather_step(2, 0)
    grad_chunk(0, 0)
    grad_chunk(0, 1)
    half_step(0, 1)
    grad_chunk(0, 2)
    half_step(1, 1)
    gather_step(3, 0)
    grad_chunk(0, 3)
    gather_step(2, 1)
    transpose_cols(1)
    grad_chunk(1, 0)
    half_step(0, 2)
    grad_chunk(1, 1)
    half_step(1, 2)
    half_step(0, 3)
    grad_chunk(1, 2)
    gather_step(3, 1)
    grad_chunk(1, 3)
    half_step(0, 4)
    gather_step(2, 2)
    half_step(1, 3)
    half_step(0, 5)
    project(0)
    half_step(1, 4)
    scatter(0)
    half_step(1, 5)
    project(1)
    scatter(1)
    moments(0)
    moments(1)
    gather_step(2, 3)
    gather_step(3, 2)
    directions(0)
    expand(0)
    directions(1)
    gather_step(2, 4)
    gather_step(3, 3)
    expand(1)
    gather_step(2, 5)
    finish_first(squares(0))
    gather_step(3, 4)
    ss[...] = squares(1)
    gather_step(3, 5)

    all_sent(F, 0)
    all_sent(W, 1)
    for k in range(2):
        remote(X, X, d_send.at[k], d_recv.at[0], partner).wait_send()
        remote(R, R, s_send.at[k], s_recv.at[0], partner).wait_send()
    ref = XR.at[:, pl.ds(0, 3)]
    remote(ref, ref, x_send.at[0], x_recv.at[0], partner).wait_send()


def finish_kernel(
    E, W, mom, ss, copy_first, own_first, w1,
    step0, upd0, fn0, sn0, copy0, step1, upd1, fn1, sn1, copy1,
    wf, stage, st, up, in_sem, sem,
):
    me = (lax.axis_index("z") * 4 + lax.axis_index("y")) * 2 + lax.axis_index("c")
    win = pltpu.make_async_copy(w1, wf, in_sem)
    win.start()
    done = []

    def out(src, dst):
        cp = pltpu.make_async_copy(src, dst, sem.at[len(done)])
        cp.start()
        done.append(cp)

    for q in range(2):
        out(copy_first.at[pl.ds(1024 * q, 1024)], copy0.at[pl.ds(1024 * q, 1024)])
    out(own_first.at[0], step0)
    out(own_first.at[1], upd0)
    for m, (fn, sn) in enumerate(((fn0, sn0), (fn1, sn1))):
        out(mom.at[m, 0], fn)
        out(mom.at[m, 1], sn)
    scale = scale_of(ss[...])
    for r in range(8):
        stage[256 * r : 256 * r + 256] = new_copy(scale, E[4 * r : 4 * r + 4], W[1, 4 * r : 4 * r + 4])
        out(stage.at[pl.ds(256 * r, 256)], copy1.at[pl.ds(256 * r, 256)])
    step = new_step(scale, E[me])
    st[...] = step
    out(st, step1)
    win.wait()
    up[...] = wf[...] - step
    out(up, upd1)
    for cp in done:
        cp.wait()


def local(
    model_input, value_cotan, mixer_cotan, head_output,
    value_weight, value_factor, value_first, value_second,
    output_weight, output_factor, output_first, output_second,
):
    any_spec = pl.BlockSpec(memory_space=pl.ANY)
    vmem_spec = pl.BlockSpec(memory_space=pltpu.VMEM)
    DMA = pltpu.SemaphoreType.DMA
    results = pl.pallas_call(
        exchange_kernel,
        out_shape=(
            pltpu.VMEM((32, 64, 512), F32),
            pltpu.VMEM((2, 32, 64, 512), BF),
            pltpu.VMEM((2, 2, 16, 512), F32),
            pltpu.VMEM((8, 128), F32),
            pltpu.VMEM((2048, 512), BF),
            pltpu.VMEM((2, 64, 512), F32),
        ),
        in_specs=[any_spec] * 12,
        out_specs=(vmem_spec,) * 6,
        scratch_shapes=[
            pltpu.VMEM((32, 64, 512), F32),
            pltpu.VMEM((2, 4, 2048, 512), BF),
            pltpu.VMEM((2, 2048, 512), BF),
            pltpu.VMEM((2, 512, 2048), BF),
            pltpu.VMEM((2, 512, 2048), BF),
            pltpu.VMEM((2, 32, 64, 512), BF),
            pltpu.VMEM((2, 64, 512), F32),
            pltpu.VMEM((4, 16, 512), F32),
            pltpu.VMEM((2, 16, 2, 16, 512), BF),
            pltpu.VMEM((2, 16, 16, 512), BF),
            pltpu.VMEM((2, 16, 16, 512), BF),
            pltpu.VMEM((2, 15, 16, 512), BF),
            pltpu.VMEM((2, 16, 2, 16, 512), BF),
            pltpu.VMEM((2, 4, 8, 128), F32),
            DMA((13,)),
            DMA((2,)),
            DMA((34,)),
            DMA((2,)),
            DMA((4,)),
            DMA((2,)),
            DMA((4,)),
            DMA((1,)),
            DMA((2,)),
        ],
        compiler_params=pltpu.CompilerParams(
            collective_id=0, has_side_effects=True, vmem_limit_bytes=44 * 1024 * 1024
        ),
        name="exchange",
    )(
        model_input, value_cotan, mixer_cotan, head_output,
        value_weight, output_weight, value_factor, output_factor,
        value_first, value_second, output_first, output_second,
    )
    shapes = []
    for _ in range(2):
        shapes += [
            jax.ShapeDtypeStruct((64, 512), F32),
            jax.ShapeDtypeStruct((64, 512), F32),
            jax.ShapeDtypeStruct((16, 512), F32),
            jax.ShapeDtypeStruct((16, 512), F32),
            jax.ShapeDtypeStruct((2048, 512), BF),
        ]
    return pl.pallas_call(
        finish_kernel,
        out_shape=tuple(shapes),
        in_specs=[vmem_spec] * 6 + [any_spec],
        out_specs=(any_spec,) * 10,
        scratch_shapes=[
            pltpu.VMEM((64, 512), F32),
            pltpu.VMEM((2048, 512), BF),
            pltpu.VMEM((64, 512), F32),
            pltpu.VMEM((64, 512), F32),
            DMA,
            DMA((18,)),
        ],
        compiler_params=pltpu.CompilerParams(vmem_limit_bytes=8 * 1024 * 1024),
        name="finish",
    )(*results, output_weight)


def solution(mesh):
    torus = Mesh(mesh.devices.reshape(4, 4, 2, mesh.shape["tp"]), ("z", "y", "c", "x"))
    rows, cols = P(FS, None), P(FS, "x")
    part = (cols, cols, cols, cols, P(None, "x"))
    return jax.shard_map(
        local, mesh=torus,
        in_specs=(rows, cols, rows, cols, cols, rows, cols, cols, cols, rows, cols, cols),
        out_specs=part + part, check_vma=False,
    )
```

```python
import functools

import jax
import jax.numpy as jnp
from jax import lax
from jax.experimental import pallas as pl
from jax.experimental.pallas import tpu as pltpu
from jax.sharding import Mesh
from jax.sharding import PartitionSpec as P

D = 2048
HV = 2048
FS = ("z", "y", "c")
MESH = pl.DeviceIdType.MESH

beta_first = 0.8
beta_second = 0.9
step_rate = 0.02
scale_floor = 0.25
tiny_eps = 1e-08

BF = jnp.bfloat16
F32 = jnp.float32


def scale_of(squares):
    mean_square = jnp.sum(squares) / (D * HV)
    return step_rate / jnp.sqrt(jnp.full((8, 512), mean_square, F32) + scale_floor)


def new_step(scale, expanded):
    return (scale[None] * expanded.reshape(-1, 8, 512)).reshape(-1, 512)


def new_copy(scale, expanded, weight):
    return (weight.reshape(-1, 512).astype(F32) - new_step(scale, expanded)).astype(BF)


def exchange_kernel(
    rows0, cols0, rows1, cols1, w0, w1, f0, f1, a0, b0, a1, b1,
    E1, W, mom, ss, copy, own,
    E0, rows, cols, colsT, gT, F, wf, mo, Pj, X, S, R, Dr, XR,
    in_sem, g_send, g_recv, d_send, d_recv, s_send, s_recv, x_send, x_recv,
):
    z, y, c, x = (lax.axis_index(n) for n in ("z", "y", "c", "x"))
    chip = z * 4 + y
    other = 1 - c
    ra = y + c * (z - y)
    rb = z + c * (y - z)

    def place(a, b):
        zz = b + c * (a - b)
        yy = a + c * (b - a)
        return zz, yy

    def shard(a, b):
        zz, yy = place(a, b)
        return (zz * 4 + yy) * 2 + c

    def at(a, b):
        zz, yy = place(a, b)
        return {"z": zz, "y": yy}

    def plus(v, k):
        return lax.rem(v + k, 4)

    def remote(src, dst, ssem, rsem, dev):
        return pltpu.make_async_remote_copy(
            src_ref=src, dst_ref=dst, send_sem=ssem, recv_sem=rsem,
            device_id=dev, device_id_type=MESH,
        )

    partner = {"c": other}

    bar = pltpu.get_barrier_semaphore()
    peers = [{"z": plus(z, k)} for k in range(1, 4)] + [{"y": plus(y, k)} for k in range(1, 4)]
    xpeers = [{"x": plus(x, k)} for k in range(1, 4)]
    for p in peers + [partner] + xpeers:
        pl.semaphore_signal(bar, inc=1, device_id=p, device_id_type=MESH)

    me = chip * 2 + c
    fin = [pltpu.make_async_copy(f, F.at[m, me], in_sem.at[0]) for m, f in enumerate((f0, f1))]
    win = [pltpu.make_async_copy(w, wf.at[m], in_sem.at[1]) for m, w in enumerate((w0, w1))]
    cin = [pltpu.make_async_copy(v, cols.at[m], in_sem.at[2 + m]) for m, v in enumerate((cols0, cols1))]
    rin = [
        [
            pltpu.make_async_copy(
                v.at[:, pl.ds(512 * j, 512)], rows.at[m, j], in_sem.at[4 + j]
            )
            for j in range(4)
        ]
        for m, v in enumerate((rows0, rows1))
    ]
    min_ = [
        pltpu.make_async_copy(v, mo.at[i], in_sem.at[8]) for i, v in enumerate((a0, b0, a1, b1))
    ]
    for cp in fin + [cin[0]] + win + rin[0] + [cin[1]] + min_:
        cp.start()

    def loaded(ref, k):
        pltpu.make_async_copy(ref, ref, in_sem.at[k]).wait()

    def G(p):
        return W.at[p - 2]

    am, ap, af = plus(ra, 3), plus(ra, 1), plus(ra, 2)
    bm, bp, bf = plus(rb, 3), plus(rb, 1), plus(rb, 2)
    LO, HI = pl.ds(0, 32), pl.ds(32, 32)

    def send(p, s, dev, k, half=None):
        ref = G(p).at[s] if half is None else G(p).at[s, half]
        remote(ref, ref, g_send.at[1], g_recv.at[6 + 7 * p + k], dev).start()

    def arrived(p, k, n):
        ref = G(p).at[pl.ds(0, n)]
        remote(ref, ref, g_send.at[1], g_recv.at[6 + 7 * p + k], partner).wait_recv()

    def across(p, s):
        send(p, s, partner, 6)

    def gather_step(p, step):
        if step == 0:
            s = shard(ra, rb)
            send(p, s, at(ap, rb), 0)
            send(p, s, at(am, rb), 0)
            send(p, s, at(ra, bp), 2)
            send(p, s, at(ra, bm), 2)
            across(p, s)
        if step == 1:
            arrived(p, 0, 2)
            send(p, shard(am, rb), at(ap, rb), 1, LO)
            send(p, shard(ap, rb), at(am, rb), 1, HI)
            for a in (am, ap):
                send(p, shard(a, rb), at(ra, bp), 3)
                send(p, shard(a, rb), at(ra, bm), 3)
            arrived(p, 2, 2)
            send(p, shard(ra, bm), at(ra, bp), 5, LO)
            send(p, shard(ra, bp), at(ra, bm), 5, HI)
            for s in (shard(am, rb), shard(ap, rb), shard(ra, bm), shard(ra, bp)):
                across(p, s)
        if step == 2:
            arrived(p, 1, 1)
            send(p, shard(af, rb), at(ra, bp), 4)
            send(p, shard(af, rb), at(ra, bm), 4)
            arrived(p, 3, 4)
            for a in (am, ap):
                send(p, shard(a, bm), at(ra, bp), 5, LO)
                send(p, shard(a, bp), at(ra, bm), 5, HI)
            across(p, shard(af, rb))
            for a in (am, ap):
                across(p, shard(a, bm))
                across(p, shard(a, bp))
        if step == 3:
            arrived(p, 4, 2)
            send(p, shard(af, bm), at(ra, bp), 5, LO)
            send(p, shard(af, bp), at(ra, bm), 5, HI)
            across(p, shard(af, bm))
            across(p, shard(af, bp))
        if step == 4:
            arrived(p, 5, 4)
            for a in (ra, am, ap, af):
                across(p, shard(a, bf))
        if step == 5:
            arrived(p, 6, 16)

    mine = pl.ds(32 * lax.rem(x, 2), 32)
    xp, xm = {"x": plus(x, 1)}, {"x": plus(x, 3)}

    theirs = pl.ds(32 - 32 * lax.rem(x, 2), 32)

    def send_half(p, s, dev, k):
        ref = F.at[p, s, mine]
        remote(ref, ref, g_send.at[0], g_recv.at[10 * p + k], dev).start()

    def halves(p, k, n):
        ref = F.at[p, pl.ds(0, n), pl.ds(0, 32)]
        remote(ref, ref, g_send.at[0], g_recv.at[10 * p + k], partner).wait_recv()

    def over(p, s, part=None):
        ref = F.at[p, s] if part is None else F.at[p, s, part]
        remote(ref, ref, g_send.at[0], g_recv.at[10 * p + 7], partner).start()

    def half_step(p, step):
        if step == 0:
            s = shard(ra, rb)
            for k, a in ((2, af), (0, ap), (1, am)):
                send_half(p, s, at(a, rb), k)
            for b in (bf, bp, bm):
                send_half(p, s, at(ra, b), 3)
            over(p, s)
        if step == 1:
            for k, a, dev in ((0, am, xp), (1, ap, xm), (2, af, xp)):
                halves(p, k, 1)
                s = shard(a, rb)
                for q, b in ((6, bf), (4, bp), (5, bm)):
                    send_half(p, s, at(ra, b), q)
                send_half(p, s, dev, 8)
                over(p, s, mine)
            halves(p, 3, 3)
            for b, dev in ((bm, xm), (bp, xp), (bf, xm)):
                send_half(p, shard(ra, b), dev, 8)
                over(p, shard(ra, b), mine)
        if step == 2:
            for k, b, f in ((4, bm, 0), (5, bp, 1), (6, bf, 0)):
                halves(p, k, 3)
                for n, a in enumerate((am, ap, af)):
                    send_half(p, shard(a, b), xp if (n + f) % 2 else xm, 9)
                    over(p, shard(a, b), mine)
        if step == 3:
            halves(p, 8, 6)
            for s in [shard(a, rb) for a in (am, ap, af)] + [shard(ra, b) for b in (bm, bp, bf)]:
                over(p, s, theirs)
        if step == 4:
            halves(p, 9, 9)
            for b in (bm, bp, bf):
                for a in (am, ap, af):
                    over(p, shard(a, b), theirs)
        if step == 5:
            ref = F.at[p, pl.ds(0, 16)]
            remote(ref, ref, g_send.at[0], g_recv.at[10 * p + 7], partner).wait_recv()

    def all_sent(array, k):
        ref = array.at[:, pl.ds(0, 31)]
        remote(ref, ref, g_send.at[k], g_recv.at[0], partner).wait_send()

    def round_weights():
        loaded(wf, 1)
        for m in range(2):
            W[m, me] = wf[m].astype(BF)

    def transpose_cols(m):
        cin[m].wait()
        for t in range(4):
            colsT[m, :, 512 * t : 512 * t + 512] = cols[m, 512 * t : 512 * t + 512, :].T

    def grad_chunk(m, j):
        rin[m][j].wait()
        if m == 0:
            rin[1][j].start()
        out = jnp.dot(colsT[m], rows[m, j], preferred_element_type=F32)
        gT[m, :, 512 * j : 512 * j + 512] = out.astype(BF)

    def to_partner(m):
        return remote(Pj.at[m, :, other], X.at[m], d_send.at[0], d_recv.at[m], partner)

    def project(m):
        for n in range(2):
            f = F[m, :, :, 256 * n : 256 * n + 256].reshape(D, 256)
            out = jnp.dot(gT[m], f, preferred_element_type=F32)
            Pj[m, 8 * n : 8 * n + 8] = out.T.astype(BF).reshape(8, 2, 16, 512)
        to_partner(m).start()

    FAR_FIRST = (10, 9, 11, 6, 14, 2, 8, 5, 7, 13, 15, 1, 3, 4, 12)

    def scatter(m):
        to_partner(m).wait_recv()
        S[m] = (Pj[m, :, c].astype(F32) + X[m].astype(F32)).astype(BF)
        for k in FAR_FIRST:
            zz, yy = plus(z, k // 4), plus(y, k % 4)
            remote(
                S.at[m, zz * 4 + yy], R.at[m, k - 1], s_send.at[0], s_recv.at[m],
                {"z": zz, "y": yy},
            ).start()

    def moments(m):
        if m == 0:
            loaded(mo, 8)
        remote(R.at[m], R.at[m], s_send.at[0], s_recv.at[m], partner).wait_recv()
        proj = S[m, chip].astype(F32) + jnp.sum(R[m].astype(F32), axis=0)
        fnew = beta_first * mo[2 * m] + (1.0 - beta_first) * proj
        snew = beta_second * mo[2 * m + 1] + (1.0 - beta_second) * proj * proj
        mom[m, 0] = fnew
        mom[m, 1] = snew
        Dr[m, chip, c] = (fnew / (jnp.sqrt(snew) + tiny_eps)).astype(BF)
        ref = Dr.at[m, chip, c]
        for k in FAR_FIRST:
            zz, yy = plus(z, k // 4), plus(y, k % 4)
            remote(ref, ref, s_send.at[1], s_recv.at[2 + m], {"z": zz, "y": yy}).start()

    def directions(m):
        remote(R.at[m], R.at[m], s_send.at[1], s_recv.at[2 + m], partner).wait_recv()
        ref = Dr.at[m, :, c]
        remote(ref, ref, d_send.at[1], d_recv.at[2 + m], partner).start()

    def expand(m):
        ref = Dr.at[m, :, other]
        remote(ref, ref, d_send.at[1], d_recv.at[2 + m], partner).wait_recv()
        direction = Dr[m].reshape(512, 512)
        total = jnp.zeros((8, 512), F32)
        for r in range(4):
            f = F[m, 8 * r : 8 * r + 8].reshape(512, 512)
            e = jnp.dot(f, direction, preferred_element_type=F32)
            (E0, E1)[m][8 * r : 8 * r + 8] = e.reshape(8, 64, 512)
            total = total + jnp.sum((e * e).reshape(64, 8, 512), axis=0)
        part = total[:, :128] + total[:, 128:256] + total[:, 256:384] + total[:, 384:]
        XR[m, x] = part
        ref = XR.at[m, x]
        for p in xpeers:
            remote(ref, ref, x_send.at[0], x_recv.at[m], p).start()

    def squares(m):
        ref = XR.at[m, pl.ds(0, 3)]
        remote(ref, ref, x_send.at[0], x_recv.at[m], partner).wait_recv()
        return (XR[m, 0] + XR[m, 1]) + (XR[m, 2] + XR[m, 3])

    def finish_first(total):
        scale = scale_of(total)
        for r in range(8):
            copy[256 * r : 256 * r + 256] = new_copy(scale, E0[4 * r : 4 * r + 4], W[0, 4 * r : 4 * r + 4])
        step = new_step(scale, E0[me])
        own[0] = step
        own[1] = wf[0] - step

    loaded(F.at[:, me], 0)
    pl.semaphore_wait(bar, 10)
    half_step(0, 0)
    half_step(1, 0)
    transpose_cols(0)
    round_weights()
    gather_step(2, 0)
    grad_chunk(0, 0)
    grad_chunk(0, 1)
    half_step(0, 1)
    grad_chunk(0, 2)
    half_step(1, 1)
    gather_step(3, 0)
    grad_chunk(0, 3)
    gather_step(2, 1)
    transpose_cols(1)
    grad_chunk(1, 0)
    half_step(0, 2)
    grad_chunk(1, 1)
    half_step(1, 2)
    half_step(0, 3)
    grad_chunk(1, 2)
    gather_step(3, 1)
    gather_step(2, 2)
    grad_chunk(1, 3)
    half_step(0, 4)
    half_step(1, 3)
    half_step(0, 5)
    project(0)
    half_step(1, 4)
    scatter(0)
    half_step(1, 5)
    project(1)
    scatter(1)
    gather_step(2, 3)
    moments(0)
    moments(1)
    gather_step(3, 2)
    directions(0)
    expand(0)
    directions(1)
    gather_step(2, 4)
    gather_step(3, 3)
    expand(1)
    gather_step(2, 5)
    finish_first(squares(0))
    gather_step(3, 4)
    ss[...] = squares(1)
    gather_step(3, 5)

    all_sent(F, 0)
    all_sent(W, 1)
    for k in range(2):
        remote(X, X, d_send.at[k], d_recv.at[0], partner).wait_send()
        remote(R, R, s_send.at[k], s_recv.at[0], partner).wait_send()
    ref = XR.at[:, pl.ds(0, 3)]
    remote(ref, ref, x_send.at[0], x_recv.at[0], partner).wait_send()


def finish_kernel(
    E, W, mom, ss, copy_first, own_first, w1,
    step0, upd0, fn0, sn0, copy0, step1, upd1, fn1, sn1, copy1,
    wf, stage, st, in_sem, sem,
):
    me = (lax.axis_index("z") * 4 + lax.axis_index("y")) * 2 + lax.axis_index("c")
    win = pltpu.make_async_copy(w1, wf, in_sem)
    win.start()

    def out(src, dst, k):
        pltpu.make_async_copy(src, dst, sem.at[k]).start()

    out(copy_first, copy0, 0)
    out(own_first.at[0], step0, 1)
    out(own_first.at[1], upd0, 1)
    for m, (fn, sn) in enumerate(((fn0, sn0), (fn1, sn1))):
        out(mom.at[m, 0], fn, 2)
        out(mom.at[m, 1], sn, 2)
    scale = scale_of(ss[...])
    for r in range(8):
        stage[256 * r : 256 * r + 256] = new_copy(scale, E[4 * r : 4 * r + 4], W[1, 4 * r : 4 * r + 4])
        out(stage.at[pl.ds(256 * r, 256)], copy1.at[pl.ds(256 * r, 256)], 3)
    step = new_step(scale, E[me])
    st[0] = step
    out(st.at[0], step1, 4)
    win.wait()
    st[1] = wf[...] - step
    out(st.at[1], upd1, 4)
    for k, ref in enumerate((copy_first, own_first, mom, stage, st)):
        pltpu.make_async_copy(ref, ref, sem.at[k]).wait()


def local(
    model_input, value_cotan, mixer_cotan, head_output,
    value_weight, value_factor, value_first, value_second,
    output_weight, output_factor, output_first, output_second,
):
    any_spec = pl.BlockSpec(memory_space=pl.ANY)
    vmem_spec = pl.BlockSpec(memory_space=pltpu.VMEM)
    DMA = pltpu.SemaphoreType.DMA
    results = pl.pallas_call(
        exchange_kernel,
        out_shape=(
            pltpu.VMEM((32, 64, 512), F32),
            pltpu.VMEM((2, 32, 64, 512), BF),
            pltpu.VMEM((2, 2, 16, 512), F32),
            pltpu.VMEM((8, 128), F32),
            pltpu.VMEM((2048, 512), BF),
            pltpu.VMEM((2, 64, 512), F32),
        ),
        in_specs=[any_spec] * 12,
        out_specs=(vmem_spec,) * 6,
        scratch_shapes=[
            pltpu.VMEM((32, 64, 512), F32),
            pltpu.VMEM((2, 4, 2048, 512), BF),
            pltpu.VMEM((2, 2048, 512), BF),
            pltpu.VMEM((2, 512, 2048), BF),
            pltpu.VMEM((2, 512, 2048), BF),
            pltpu.VMEM((2, 32, 64, 512), BF),
            pltpu.VMEM((2, 64, 512), F32),
            pltpu.VMEM((4, 16, 512), F32),
            pltpu.VMEM((2, 16, 2, 16, 512), BF),
            pltpu.VMEM((2, 16, 16, 512), BF),
            pltpu.VMEM((2, 16, 16, 512), BF),
            pltpu.VMEM((2, 15, 16, 512), BF),
            pltpu.VMEM((2, 16, 2, 16, 512), BF),
            pltpu.VMEM((2, 4, 8, 128), F32),
            DMA((9,)),
            DMA((2,)),
            DMA((34,)),
            DMA((2,)),
            DMA((4,)),
            DMA((2,)),
            DMA((4,)),
            DMA((1,)),
            DMA((2,)),
        ],
        compiler_params=pltpu.CompilerParams(
            collective_id=0, has_side_effects=True, vmem_limit_bytes=44 * 1024 * 1024
        ),
        name="exchange",
    )(
        model_input, value_cotan, mixer_cotan, head_output,
        value_weight, output_weight, value_factor, output_factor,
        value_first, value_second, output_first, output_second,
    )
    shapes = []
    for _ in range(2):
        shapes += [
            jax.ShapeDtypeStruct((64, 512), F32),
            jax.ShapeDtypeStruct((64, 512), F32),
            jax.ShapeDtypeStruct((16, 512), F32),
            jax.ShapeDtypeStruct((16, 512), F32),
            jax.ShapeDtypeStruct((2048, 512), BF),
        ]
    return pl.pallas_call(
        finish_kernel,
        out_shape=tuple(shapes),
        in_specs=[vmem_spec] * 6 + [any_spec],
        out_specs=(any_spec,) * 10,
        scratch_shapes=[
            pltpu.VMEM((64, 512), F32),
            pltpu.VMEM((2048, 512), BF),
            pltpu.VMEM((2, 64, 512), F32),
            DMA,
            DMA((5,)),
        ],
        compiler_params=pltpu.CompilerParams(vmem_limit_bytes=8 * 1024 * 1024),
        name="finish",
    )(*results, output_weight)


def solution(mesh):
    torus = Mesh(mesh.devices.reshape(4, 4, 2, mesh.shape["tp"]), ("z", "y", "c", "x"))
    rows, cols = P(FS, None), P(FS, "x")
    part = (cols, cols, cols, cols, P(None, "x"))
    return jax.shard_map(
        local, mesh=torus,
        in_specs=(rows, cols, rows, cols, cols, rows, cols, cols, cols, rows, cols, cols),
        out_specs=part + part, check_vma=False,
    )
```
